128 devices in a mesh: fs: 16 (over z, y), tp: 8 (over x, core).
Axes of the slice: x: 4, y: 4, z: 4, core: 2. Of those that a mesh axis runs over, the one named last changes fastest.
Arguments:
- tokens: bfloat16 [12288, 2048], P('fs'), may hold values from -6 to 6
- routes: int32 [12288, 2], P('fs'), may hold values from 0 to 15, all different within a row; in each aligned block of 768 rows (0 to 767, 768 to 1535, ...) at most 216 rows name the same one
- route_weight: float32 [12288, 2], P('fs'), may hold values from 0.2 to 1
- norm_gain: float32 [2048], P('fs'), may hold values from 0.1 to 1.9
- gate_master: float32 [16, 2048, 4096], P(None, 'fs', 'tp'), may hold values from -0.125 to 0.125
- up_master: float32 [16, 2048, 4096], P(None, 'fs', 'tp'), may hold values from -0.125 to 0.125
- down_master: float32 [16, 4096, 2048], P(None, 'fs', 'tp'), may hold values from -0.09375 to 0.09375
Outputs:
- gate_serve: bfloat16 [16, 2048, 4096], P('fs', None, 'tp')
- up_serve: bfloat16 [16, 2048, 4096], P('fs', None, 'tp')
- down_serve: bfloat16 [16, 4096, 2048], P('fs', 'tp')
- layer_out: bfloat16 [12288, 2048], P('fs', 'tp')
The draws below stay inside these ranges and needn't reach their ends.
Inputs may be any that keep to these rules, and one draw needn't show every extreme that they name: `routes`: each row names two different experts; among the 768 rows of one index of fs no expert is named by more than 216 rows, a bound that some block reaches.
All inputs are finite; a program needn't handle non-finite values.
Results may differ from the reference program's by a relative error of at most 0.015.
Values may be sent and summed in bfloat16 or wider, within the bound.
A program may use at most 192 MiB of HBM per device.

```python
import math
import jax
import jax.numpy as jnp
import numpy as np
from jax import lax

D = 2048
FF = 4096
TOK_DEV = 768
CAP = 216
EXPERTS = 16
TOKENS = 12288
N_FS = 16
N_TP = 8


def block_scale(key, extent, shards, low, largest):
    loudness, own = 1.0, jax.random.fold_in(key, 6)
    for axis_at, parts in shards:
        draws = jnp.exp(jax.random.uniform(jax.random.fold_in(own, axis_at), (parts,), jnp.float32, low / len(shards), largest / len(shards)))
        loudness = loudness * jnp.repeat(draws, extent[axis_at] // parts).reshape([-1 if axis == axis_at else 1 for axis in range(len(extent))])
    return loudness


def deal_out(key, own, number, rows, count, top, reach, slope):
    order = jax.random.permutation(key, count)
    crowded, usual = portions_of(count, rows * top, reach, slope, True), portions_of(count, rows * top, reach, slope, False)
    places = jnp.arange(count)

    def named(lengths, turn):
        used = int((lengths > 0).sum())
        fixed = max(1, used // 4)
        passed = fixed + (places - fixed + turn * (used - fixed)) % max(1, count - fixed)
        return jnp.zeros((count,), jnp.int32).at[order[jnp.where(places < fixed, places, passed)]].set(jnp.asarray(lengths, jnp.int32))

    lengths = jnp.where(number % 4 == 0, named(crowded, number // 4), named(usual, number - number // 4 - 1))
    mixed = jax.random.permutation(jax.random.fold_in(own, 3), count)
    donor, sink = mixed[0:count // 2 * 2:2], mixed[1:count // 2 * 2:2]
    margin = jnp.minimum(lengths[donor] - 1, reach - lengths[sink]) // 2
    margin = jnp.where((donor == order[0]) | (sink == order[0]) | (lengths[sink] == 0), 0, jnp.maximum(margin, 0))
    passed = jax.random.randint(jax.random.fold_in(own, 4), (count // 2,), 0, 1 << 20) % (margin + 1)
    lengths = lengths.at[donor].add(-passed).at[sink].add(passed)
    labels = jnp.searchsorted(jnp.cumsum(lengths), jnp.arange(rows * top), side="right").astype(jnp.int32)
    table = labels.reshape(top, rows).T
    table = table[jax.random.permutation(jax.random.fold_in(own, 1), rows)]
    turn = jax.random.randint(jax.random.fold_in(own, 2), (rows, 1), 0, top)
    return jnp.take_along_axis(table, (jnp.arange(top)[None, :] + turn) % top, axis=1)


def portions_of(count, total, reach, slope, full):
    weights = [(1 << 20) // math.isqrt(rank ** slope) + 1 for rank in range(1, count + 1)]
    largest = reach if full else min(reach, max(-(-total // count), total * weights[0] // sum(weights)))
    least = 1 if total - largest >= count - 1 else 0
    holding, rest = [largest] + [least] * (count - 1), total - largest - least * (count - 1)
    while rest > 0:
        movable = [i for i in range(1, count) if holding[i] < largest] or [i for i in range(1, count) if holding[i] < reach]
        pool, remaining = sum([weights[i] for i in movable]), rest
        for i in movable:
            extra = min(reach - holding[i], max(1, remaining * weights[i] // pool), rest)
            holding[i] = holding[i] + extra
            rest = rest - extra
    return np.array(holding)


def centred(own_key, dims, deviation, most, pieces=(), kind=jnp.bfloat16):
    result = deviation * jax.random.normal(own_key, dims, jnp.float32)
    if pieces:
        result = result * block_scale(own_key, dims, pieces, -0.22, 0.18)
    return jnp.clip(result, -most, most).astype(kind)


def setup_inputs(seed: int = 0) -> dict:
    key_of = jax.random.split(jax.random.key(seed), 8)
    tokens = centred(key_of[0], (TOKENS, D), 1.0, 6.0, ((0, 16),))
    routes_keys = jax.random.split(jax.random.fold_in(key_of[1], 1), TOKENS // TOK_DEV)
    routes_turns = jax.random.permutation(jax.random.fold_in(key_of[1], 3), TOKENS // TOK_DEV)
    routes = jax.vmap(lambda own, number: deal_out(jax.random.fold_in(key_of[1], 2), own, number, TOK_DEV, EXPERTS, 2, CAP, 2))(routes_keys, routes_turns).reshape((TOKENS, 2))
    route_weight = jnp.clip(0.2 + 0.8 * jax.random.uniform(key_of[2], (TOKENS, 2), jnp.float32) ** block_scale(key_of[2], (TOKENS, 2), ((0, 16),), -0.2, 0.2), 0.2, 1.0)
    norm_gain = jnp.clip(1.0 + 0.18 * jax.random.normal(key_of[3], (D,), jnp.float32), 0.1, 1.9)
    gate_master = centred(key_of[4], (EXPERTS, D, FF), D ** -0.5, 0.125, ((1, 16), (2, 8)), jnp.float32)
    up_master = centred(key_of[5], (EXPERTS, D, FF), D ** -0.5, 0.125, ((1, 16), (2, 8)), jnp.float32)
    down_master = centred(key_of[6], (EXPERTS, FF, D), FF ** -0.5, 0.09375, ((1, 16), (2, 8)), jnp.float32)
    return dict(tokens=tokens, routes=routes, route_weight=route_weight, norm_gain=norm_gain, gate_master=gate_master, up_master=up_master, down_master=down_master)


def reference(tokens, routes, route_weight, norm_gain, gate_master, up_master, down_master):
    values = tokens.astype(jnp.float32)
    normed = (values * lax.rsqrt(lax.optimization_barrier(jnp.mean(values * values, axis=-1, keepdims=True)) + 1e-06)).astype(jnp.bfloat16)
    gate_serve = (norm_gain[None, :, None] * gate_master).astype(jnp.bfloat16)
    up_serve = (norm_gain[None, :, None] * up_master).astype(jnp.bfloat16)
    down_serve = down_master.astype(jnp.bfloat16)
    rows_cap = N_FS * CAP
    group_units = FF // N_TP

    def expert_step(totals, expert):
        is_routed = jnp.any(routes == expert, axis=1)
        ordering = jnp.argsort(jnp.where(is_routed, 0, 1).astype(jnp.int32), stable=True)[:rows_cap]
        present = is_routed[ordering]
        chosen_rows = jnp.where(present[:, None], normed[ordering], jnp.zeros((), jnp.bfloat16))
        gate_pre = jnp.dot(chosen_rows, gate_serve[expert], preferred_element_type=jnp.float32)
        up_pre = jnp.dot(chosen_rows, up_serve[expert], preferred_element_type=jnp.float32)
        hidden = (jax.nn.silu(gate_pre) * up_pre).astype(jnp.bfloat16)
        block_sums = jnp.einsum('rgf,gfd->grd', hidden.reshape(rows_cap, N_TP, group_units).astype(jnp.float32), down_serve[expert].reshape(N_TP, group_units, D).astype(jnp.float32))
        rounded = lax.optimization_barrier(block_sums.astype(jnp.bfloat16)).astype(jnp.float32)
        expert_out = lax.optimization_barrier(jnp.sum(rounded, axis=0)).astype(jnp.bfloat16)
        row_weight = lax.optimization_barrier(jnp.sum(jnp.where(routes[ordering] == expert, route_weight[ordering], jnp.zeros((), jnp.float32)), axis=1))
        row_weight = jnp.where(present, row_weight, jnp.zeros((), jnp.float32))
        totals = totals.at[ordering].add(row_weight[:, None] * expert_out.astype(jnp.float32))
        return (totals, None)
    totals, _ = lax.scan(expert_step, jnp.zeros((TOKENS, D), jnp.float32), jnp.arange(EXPERTS, dtype=jnp.int32))
    return (gate_serve, up_serve, down_serve, totals.astype(jnp.bfloat16))
```

```python
import functools

import jax
import jax.numpy as jnp
from jax import lax
from jax.experimental import pallas as pl
from jax.experimental.pallas import tpu as pltpu
from jax.sharding import PartitionSpec as P

CAP = 216
MESH = pl.DeviceIdType.MESH
BF = jnp.bfloat16
F32 = jnp.float32
EARLY = 7


def kernel(
    tok_h, rt_ref, wt_ref, gain_ref, gate_h, up_h, down_h,
    gate_o, up_o, down_o, out_ref,
    X, RB, D2, FA, FB, RET, PS, H,
    gate_s, up_s, down_s, gate_r, up_r, down_r,
    st_a, st_d, tok, nrm, acc, pos_e, cols,
    ld, gs, gr, us, ur, ds, dr, ps, xr, ag,
    dds, ddr, s2s, s2r, sas, sar, sbs, sbr, rts, rtr, osem,
):
    fs, tp = lax.axis_index("fs"), lax.axis_index("tp")
    z, y = fs // 4, fs % 4
    x, c = tp // 2, tp % 2
    oc = 1 - c

    def to(s):
        dy = s % 4
        dz = (s // 4 + dy) % 4
        return ((z + dz) % 4) * 4 + (y + dy) % 4

    def of(s):
        dy = s % 4
        dz = (s // 4 + dy) % 4
        return ((z + 4 - dz) % 4) * 4 + (y + 4 - dy) % 4

    def at_x(d):
        return (x + d) % 4

    def lane(d, core):
        return at_x(d) * 2 + core

    sib = (fs, x * 2 + oc)

    def rc(src, dst, ss, rs, dev):
        return pltpu.make_async_remote_copy(
            src_ref=src, dst_ref=dst, send_sem=ss, recv_sem=rs, device_id=dev, device_id_type=MESH
        )

    l_gate = pltpu.make_async_copy(gate_h, st_a, ld.at[0])
    l_tok = pltpu.make_async_copy(tok_h, tok, ld.at[1])
    l_down = pltpu.make_async_copy(down_h, st_d, ld.at[2])
    l_up = pltpu.make_async_copy(up_h, st_a, ld.at[3])
    l_gate.start()
    l_tok.start()
    l_down.start()

    bar = pltpu.get_barrier_semaphore()

    def sig(dev):
        pl.semaphore_signal(bar, inc=1, device_id=dev, device_id_type=MESH)

    self_down = fs // 2 == tp

    @pl.loop(1, 16)
    def _(s):
        sig((to(s), tp))
        sig((to(s), fs // 2))

    sig(sib)
    sig((fs, lane(1, c)))
    sig((fs, lane(3, c)))

    @pl.when(jnp.logical_not(self_down))
    def _():
        sig((fs, fs // 2))

    @pl.loop(0, 16)
    def _(k):
        i, j = tp * 2 + k // 8, k % 8

        @pl.when(jnp.logical_or(i != fs, j != tp))
        def _():
            sig((i, j))

    e_id = lax.broadcasted_iota(jnp.int32, (16, 768), 0)
    m0 = e_id == rt_ref[0:1, :]
    m1 = e_id == rt_ref[1:2, :]
    mt = jnp.logical_or(m0, m1)
    before = (
        lax.broadcasted_iota(jnp.int32, (768, 768), 0) < lax.broadcasted_iota(jnp.int32, (768, 768), 1)
    )
    count = jnp.dot(
        jnp.where(mt, 1.0, 0.0).astype(BF), jnp.where(before, 1.0, 0.0).astype(BF), preferred_element_type=F32
    )
    pos_e[...] = jnp.where(mt, count, -1.0)
    slot = count + (e_id * CAP).astype(F32)
    slot0 = jnp.sum(jnp.where(m0, slot, 0.0), axis=0, keepdims=True)
    slot1 = jnp.sum(jnp.where(m1, slot, 0.0), axis=0, keepdims=True)
    row = lax.broadcasted_iota(jnp.int32, (128, 768), 0)
    table = jnp.where(
        row == 0, slot0, jnp.where(row == 1, slot1, jnp.where(row == 2, wt_ref[0:1, :], wt_ref[1:2, :]))
    )
    cols[...] = table.T

    r128 = lax.broadcasted_iota(jnp.int32, (128, 128), 0)
    c128 = lax.broadcasted_iota(jnp.int32, (128, 128), 1)
    gain = jnp.sum(jnp.where(r128 == c128, gain_ref[...], 0.0), axis=1, keepdims=True)
    mine = pl.ds(pl.multiple_of(fs * 128, 128), 128)

    l_gate.wait()

    @pl.loop(0, 16)
    def _(e):
        gate_s[e] = (st_a[e] * gain).astype(BF)

    gate_r[mine, :] = gate_s[fs]
    l_up.start()

    @pl.when(self_down)
    def _():
        pl.semaphore_wait(bar, 48)

    @pl.when(jnp.logical_not(self_down))
    def _():
        pl.semaphore_wait(bar, 50)

    def gate_copy(s):
        return rc(gate_s.at[to(s)], gate_r.at[mine], gs.at[s], gr.at[fs], (to(s), tp))

    def up_copy(s):
        return rc(up_s.at[to(s)], up_r.at[mine], us.at[s], ur.at[fs], (to(s), tp))

    def down_copy(s):
        return rc(
            down_s.at[to(s)], down_r.at[fs % 2, tp], ds.at[s], dr.at[(fs % 2) * 8 + tp], (to(s), fs // 2)
        )

    @pl.loop(1, 1 + EARLY)
    def _(s):
        gate_copy(s).start()

    l_tok.wait()
    share = pl.ds(pl.multiple_of(tp * 256, 256), 256)

    @pl.loop(0, 12)
    def _(r):
        rows = pl.ds(pl.multiple_of(r * 64, 64), 64)
        v = tok[rows, :].astype(F32)
        inv = lax.rsqrt(jnp.mean(v * v, axis=-1, keepdims=True) + 1e-06)
        nrm[rows, :] = (tok[rows, share].astype(F32) * inv).astype(BF)

    s_id = lax.broadcasted_iota(jnp.int32, (CAP, 768), 0).astype(F32)

    def block(e):
        pick = jnp.where(s_id == pos_e[pl.ds(e, 1), :], 1.0, 0.0).astype(BF)
        return jnp.dot(pick, nrm[...], preferred_element_type=F32).astype(BF)

    def disp_copy(s):
        return rc(PS.at[s], X.at[fs, x, c], ps.at[s], xr.at[fs * 8 + tp], (to(s), tp))

    X[fs, x, c] = block(fs)

    @pl.loop(1, 17)
    def _(s):
        @pl.when(s < 16)
        def _():
            PS[s] = block(to(s))

        @pl.when(s > 1)
        def _():
            disp_copy(s - 1).start()

    @pl.loop(1 + EARLY, 16)
    def _(s):
        gate_copy(s).start()

    l_up.wait()

    @pl.loop(0, 16)
    def _(e):
        up_s[e] = (st_a[e] * gain).astype(BF)

    up_r[mine, :] = up_s[fs]

    @pl.loop(1, 16)
    def _(s):
        up_copy(s).start()

    l_down.wait()

    @pl.loop(0, 16)
    def _(e):
        down_s[e] = st_d[e].astype(BF)

    @pl.loop(1, 16)
    def _(s):
        down_copy(s).start()

    @pl.when(jnp.logical_not(self_down))
    def _():
        down_copy(0).start()

    @pl.when(self_down)
    def _():
        down_r[fs % 2, tp] = down_s[fs]

    def ag_copy(s, d, core, k, dev):
        i = of(s)
        p = at_x(d)
        return rc(X.at[i, p, core], X.at[i, p, core], ag.at[s * 7 + k], xr.at[i * 8 + p * 2 + core], dev)

    def ag_wait(s, d, core):
        ag_copy(s, d, core, 0, sib).wait_recv()

    def ahead(s):
        return 1 + 2 * (s % 2)

    @pl.loop(0, 20)
    def _(t):
        @pl.when(t < 16)
        def _():
            @pl.when(t > 0)
            def _():
                ag_wait(t, 0, c)

            ag_copy(t, 0, c, 0, (fs, lane(1, c))).start()
            ag_copy(t, 0, c, 1, (fs, lane(3, c))).start()
            ag_copy(t, 0, c, 2, sib).start()

        @pl.when(jnp.logical_and(t >= 2, t < 18))
        def _():
            s = t - 2
            da = ahead(s)
            ag_wait(s, 4 - da, c)
            ag_copy(s, 4 - da, c, 3, (fs, lane(da, c))).start()
            ag_copy(s, 4 - da, c, 4, sib).start()
            ag_wait(s, da, c)
            ag_copy(s, da, c, 5, sib).start()

        @pl.when(t >= 4)
        def _():
            s = t - 4
            ag_wait(s, 2, c)
            ag_copy(s, 2, c, 6, sib).start()

    @pl.loop(1, 16)
    def _(s):
        i = of(s)
        rows = pl.ds(pl.multiple_of(i * 128, 128), 128)
        rc(gate_s.at[0], gate_r.at[rows], gs.at[0], gr.at[i], sib).wait_recv()
        rc(up_s.at[0], up_r.at[rows], us.at[0], ur.at[i], sib).wait_recv()

    o_gate = pltpu.make_async_copy(gate_r, gate_o.at[0], osem.at[16])
    o_up = pltpu.make_async_copy(up_r, up_o.at[0], osem.at[17])
    o_gate.start()
    o_up.start()

    @pl.loop(0, 16)
    def _(s):
        i = of(s)
        for d in range(4):
            ag_wait(s, d, oc)
        rows = jnp.concatenate([X[i, p // 2, p % 2] for p in range(8)], axis=1)
        for h in range(2):
            g = jnp.dot(rows, gate_r[:, h * 256 : h * 256 + 256], preferred_element_type=F32)
            u = jnp.dot(rows, up_r[:, h * 256 : h * 256 + 256], preferred_element_type=F32)
            H[s, h] = (g / (1.0 + jnp.exp(-g)) * u).astype(BF)

    @pl.loop(0, 16)
    def _(k):
        h, j = k // 8, k % 8
        i = tp * 2 + h

        @pl.when(jnp.logical_or(i != fs, j != tp))
        def _():
            rc(down_s.at[0], down_r.at[h, j], ds.at[0], dr.at[k], sib).wait_recv()

    def o_down(k):
        h, j = k // 8, k % 8
        return pltpu.make_async_copy(
            down_r.at[h, j], down_o.at[0, pl.ds(h * 256, 256), pl.ds(j * 256, 256)], osem.at[k]
        )

    for k in range(16):
        o_down(k).start()

    acc[...] = jnp.zeros_like(acc)

    def pair_copy(s):
        return rc(X.at[of(s), :, oc], RB.at[s], dds.at[s], ddr.at[s], sib)

    def far_copy(s):
        return rc(X.at[of(s), at_x(2), c], D2.at[s], s2s.at[s], s2r.at[s], (fs, lane(ahead(s), c)))

    def a_copy(s):
        return rc(
            X.at[of(s), at_x(ahead(s)), c], FA.at[s], sas.at[s], sar.at[s], (fs, lane(ahead(s), c))
        )

    def b_copy(s):
        return rc(
            X.at[of(s), at_x(4 - ahead(s)), c], FB.at[s], sbs.at[s], sbr.at[s], (fs, lane(4 - ahead(s), c))
        )

    def ret_copy(s):
        return rc(X.at[of(s), x, c], RET.at[fs], rts.at[s], rtr.at[fs], (of(s), tp))

    LAGS = (0, 1, 3, 5, 8)

    def stage(t, k, low=0):
        s = t - LAGS[k]
        return jnp.logical_and(s >= low, s < 16), s

    @pl.loop(0, 16 + LAGS[4])
    def _(t):
        on3, s3 = stage(t, 3)
        on2, s2 = stage(t, 2)
        on1, s1 = stage(t, 1)
        on0, s0 = stage(t, 0)
        on4, s4 = stage(t, 4)

        @pl.when(on3)
        def _():
            a_copy(s3).wait_recv()
            b_copy(s3).wait_recv()
            i = of(s3)
            X[i, x, c] = (X[i, x, c].astype(F32) + FA[s3].astype(F32) + FB[s3].astype(F32)).astype(BF)

        @pl.when(on2)
        def _():
            far_copy(s2).wait_recv()
            i, p = of(s2), at_x(ahead(s2))
            X[i, p, c] = (X[i, p, c].astype(F32) + D2[s2].astype(F32)).astype(BF)

        @pl.when(on1)
        def _():
            pair_copy(s1).wait_recv()
            i = of(s1)
            for p in range(4):
                X[i, p, c] = (X[i, p, c].astype(F32) + RB[s1, p].astype(F32)).astype(BF)

        @pl.when(on0)
        def _():
            for k in range(7):
                ag_copy(s0, 0, c, k, sib).wait_send()
            i = of(s0)
            hid = jnp.concatenate([H[s0, 0], H[s0, 1]], axis=1)
            for j in range(8):
                w = jnp.concatenate([down_r[0, j], down_r[1, j]], axis=0)
                X[i, j // 2, j % 2] = jnp.dot(hid, w, preferred_element_type=F32).astype(BF)

        @pl.when(on3)
        def _():
            @pl.when(s3 > 0)
            def _():
                ret_copy(s3).start()

            @pl.when(s3 == 0)
            def _():
                RET[fs] = X[fs, x, c]

        @pl.when(on2)
        def _():
            a_copy(s2).start()

        @pl.when(on1)
        def _():
            far_copy(s1).start()
            b_copy(s1).start()

        @pl.when(on0)
        def _():
            pair_copy(s0).start()

        @pl.when(on4)
        def _():
            e = to(s4)

            @pl.when(s4 > 0)
            def _():
                rc(X.at[0, 0, 0], RET.at[e], rts.at[0], rtr.at[e], sib).wait_recv()

            want = lax.broadcasted_iota(jnp.int32, (768, CAP), 1) + e * CAP
            k0 = cols[:, 0:1].astype(jnp.int32)
            k1 = cols[:, 1:2].astype(jnp.int32)
            w = jnp.where(want == k0, cols[:, 2:3], jnp.where(want == k1, cols[:, 3:4], 0.0))
            hi = w.astype(BF)
            lo = (w - hi.astype(F32)).astype(BF)
            back = RET[e]
            acc[...] += jnp.dot(hi, back, preferred_element_type=F32) + jnp.dot(
                lo, back, preferred_element_type=F32
            )

    out_ref[...] = acc[...].astype(BF)

    o_gate.wait()
    o_up.wait()
    for k in range(16):
        o_down(k).wait()

    @pl.loop(1, 16)
    def _(s):
        gate_copy(s).wait_send()
        up_copy(s).wait_send()
        down_copy(s).wait_send()
        disp_copy(s).wait_send()
        ret_copy(s).wait_send()

    @pl.when(jnp.logical_not(self_down))
    def _():
        down_copy(0).wait_send()

    @pl.loop(0, 16)
    def _(s):
        pair_copy(s).wait_send()
        far_copy(s).wait_send()
        a_copy(s).wait_send()
        b_copy(s).wait_send()


def body(tokens, routes, route_weight, norm_gain, gate_master, up_master, down_master):
    hbm = pl.BlockSpec(memory_space=pl.ANY)
    vm = pl.BlockSpec(memory_space=pltpu.VMEM)
    dma = pltpu.SemaphoreType.DMA
    piece = (16, CAP, 256)
    return tuple(
        pl.pallas_call(
            kernel,
            name="experts",
            out_shape=(
                jax.ShapeDtypeStruct((1, 2048, 512), BF),
                jax.ShapeDtypeStruct((1, 2048, 512), BF),
                jax.ShapeDtypeStruct((1, 512, 2048), BF),
                jax.ShapeDtypeStruct((768, 256), BF),
            ),
            in_specs=[hbm, vm, vm, vm, hbm, hbm, hbm],
            out_specs=(hbm, hbm, hbm, vm),
            scratch_shapes=[
                pltpu.VMEM((16, 4, 2, CAP, 256), BF),
                pltpu.VMEM((16, 4, CAP, 256), BF),
                pltpu.VMEM(piece, BF),
                pltpu.VMEM(piece, BF),
                pltpu.VMEM(piece, BF),
                pltpu.VMEM(piece, BF),
                pltpu.VMEM(piece, BF),
                pltpu.VMEM((16, 2, CAP, 256), BF),
                pltpu.VMEM((16, 128, 512), BF),
                pltpu.VMEM((16, 128, 512), BF),
                pltpu.VMEM((16, 256, 256), BF),
                pltpu.VMEM((2048, 512), BF),
                pltpu.VMEM((2048, 512), BF),
                pltpu.VMEM((2, 8, 256, 256), BF),
                pltpu.VMEM((16, 128, 512), F32),
                pltpu.VMEM((16, 256, 256), F32),
                pltpu.VMEM((768, 2048), BF),
                pltpu.VMEM((768, 256), BF),
                pltpu.VMEM((768, 256), F32),
                pltpu.VMEM((16, 768), F32),
                pltpu.VMEM((768, 128), F32),
                dma((4,)),
                *[dma((16,))] * 7,
                dma((128,)),
                dma((112,)),
                *[dma((16,))] * 10,
                dma((18,)),
            ],
            compiler_params=pltpu.CompilerParams(
                collective_id=0, has_side_effects=True, vmem_limit_bytes=67043328
            ),
        )(
            tokens,
            routes.T,
            route_weight.T,
            norm_gain.reshape(1, 128),
            gate_master,
            up_master,
            down_master,
        )
    )


def solution(mesh):
    placed = (
        P("fs", None),
        P("fs", None),
        P("fs", None),
        P("fs"),
        P(None, "fs", "tp"),
        P(None, "fs", "tp"),
        P(None, "fs", "tp"),
    )
    return jax.shard_map(
        body,
        mesh=mesh,
        in_specs=placed,
        out_specs=(P("fs", None, "tp"), P("fs", None, "tp"), P("fs", "tp", None), P("fs", "tp")),
        check_vma=False,
    )
```

```python
import functools

import jax
import jax.numpy as jnp
from jax import lax
from jax.experimental import pallas as pl
from jax.experimental.pallas import tpu as pltpu
from jax.sharding import PartitionSpec as P

CAP = 216
MESH = pl.DeviceIdType.MESH
BF = jnp.bfloat16
F32 = jnp.float32
EARLY = 7


def kernel(
    tok_h, rt_ref, wt_ref, gain_ref, gate_h, up_h, down_h,
    gate_o, up_o, down_o, out_ref,
    X, RB, D2, FA, FB, RET, PS, H,
    gate_s, up_s, down_s, gate_r, up_r, down_r,
    DN, st_a, st_d, tok, nrm, acc, pos_e, cols,
    ld, gs, gr, us, ur, ds, dr, es, er, ps, xr, ag,
    dds, ddr, s2s, s2r, sas, sar, sbs, sbr, rts, rtr, osem,
):
    fs, tp = lax.axis_index("fs"), lax.axis_index("tp")
    z, y = fs // 4, fs % 4
    x, c = tp // 2, tp % 2
    oc = 1 - c

    def to(s):
        dy = s % 4
        dz = (s // 4 + dy) % 4
        return ((z + dz) % 4) * 4 + (y + dy) % 4

    def of(s):
        dy = s % 4
        dz = (s // 4 + dy) % 4
        return ((z + 4 - dz) % 4) * 4 + (y + 4 - dy) % 4

    def at_x(d):
        return (x + d) % 4

    def lane(d, core):
        return at_x(d) * 2 + core

    sib = (fs, x * 2 + oc)

    def rc(src, dst, ss, rs, dev):
        return pltpu.make_async_remote_copy(
            src_ref=src, dst_ref=dst, send_sem=ss, recv_sem=rs, device_id=dev, device_id_type=MESH
        )

    l_gate = pltpu.make_async_copy(gate_h, st_a, ld.at[0])
    l_tok = pltpu.make_async_copy(tok_h, tok, ld.at[1])
    l_down = pltpu.make_async_copy(down_h, st_d, ld.at[2])
    l_up = pltpu.make_async_copy(up_h, st_a, ld.at[3])
    l_gate.start()
    l_tok.start()
    l_down.start()

    bar = pltpu.get_barrier_semaphore()

    def sig(dev):
        pl.semaphore_signal(bar, inc=1, device_id=dev, device_id_type=MESH)

    @pl.loop(1, 16)
    def _(s):
        sig((to(s), tp))

    @pl.loop(1, 8)
    def _(k):
        sig((fs, (tp + k) % 8))

    e_id = lax.broadcasted_iota(jnp.int32, (16, 768), 0)
    m0 = e_id == rt_ref[0:1, :]
    m1 = e_id == rt_ref[1:2, :]
    mt = jnp.logical_or(m0, m1)
    before = (
        lax.broadcasted_iota(jnp.int32, (768, 768), 0) < lax.broadcasted_iota(jnp.int32, (768, 768), 1)
    )
    count = jnp.dot(
        jnp.where(mt, 1.0, 0.0).astype(BF), jnp.where(before, 1.0, 0.0).astype(BF), preferred_element_type=F32
    )
    pos_e[...] = jnp.where(mt, count, -1.0)
    slot = count + (e_id * CAP).astype(F32)
    slot0 = jnp.sum(jnp.where(m0, slot, 0.0), axis=0, keepdims=True)
    slot1 = jnp.sum(jnp.where(m1, slot, 0.0), axis=0, keepdims=True)
    row = lax.broadcasted_iota(jnp.int32, (128, 768), 0)
    table = jnp.where(
        row == 0, slot0, jnp.where(row == 1, slot1, jnp.where(row == 2, wt_ref[0:1, :], wt_ref[1:2, :]))
    )
    cols[...] = table.T

    r128 = lax.broadcasted_iota(jnp.int32, (128, 128), 0)
    c128 = lax.broadcasted_iota(jnp.int32, (128, 128), 1)
    gain = jnp.sum(jnp.where(r128 == c128, gain_ref[...], 0.0), axis=1, keepdims=True)
    mine = pl.ds(pl.multiple_of(fs * 128, 128), 128)

    l_gate.wait()

    @pl.loop(0, 16)
    def _(e):
        gate_s[e] = (st_a[e] * gain).astype(BF)

    gate_r[mine, :] = gate_s[fs]
    l_up.start()

    pl.semaphore_wait(bar, 22)

    def gate_copy(s):
        return rc(gate_s.at[to(s)], gate_r.at[mine], gs.at[s], gr.at[fs], (to(s), tp))

    def up_copy(s):
        return rc(up_s.at[to(s)], up_r.at[mine], us.at[s], ur.at[fs], (to(s), tp))

    def down_copy(s):
        return rc(down_s.at[to(s)], DN.at[fs], es.at[s], er.at[fs], (to(s), tp))

    def down_on(i):
        return rc(DN.at[i], down_r.at[i % 2, tp], ds.at[i], dr.at[(i % 2) * 8 + tp], (fs, i // 2))

    @pl.loop(1, 1 + EARLY)
    def _(s):
        gate_copy(s).start()

    l_tok.wait()
    share = pl.ds(pl.multiple_of(tp * 256, 256), 256)

    @pl.loop(0, 12)
    def _(r):
        rows = pl.ds(pl.multiple_of(r * 64, 64), 64)
        v = tok[rows, :].astype(F32)
        inv = lax.rsqrt(jnp.mean(v * v, axis=-1, keepdims=True) + 1e-06)
        nrm[rows, :] = (tok[rows, share].astype(F32) * inv).astype(BF)

    s_id = lax.broadcasted_iota(jnp.int32, (CAP, 768), 0).astype(F32)

    def block(e):
        pick = jnp.where(s_id == pos_e[pl.ds(e, 1), :], 1.0, 0.0).astype(BF)
        return jnp.dot(pick, nrm[...], preferred_element_type=F32).astype(BF)

    def disp_copy(s):
        return rc(PS.at[s], X.at[fs, x, c], ps.at[s], xr.at[fs * 8 + tp], (to(s), tp))

    X[fs, x, c] = block(fs)

    @pl.loop(1, 17)
    def _(s):
        @pl.when(s < 16)
        def _():
            PS[s] = block(to(s))

        @pl.when(s > 1)
        def _():
            disp_copy(s - 1).start()

    l_down.wait()

    @pl.loop(0, 16)
    def _(e):
        down_s[e] = st_d[e].astype(BF)

    @pl.loop(1, 16)
    def _(s):
        down_copy(s).start()

    DN[fs] = down_s[fs]

    l_up.wait()

    @pl.loop(0, 16)
    def _(e):
        up_s[e] = (st_a[e] * gain).astype(BF)

    up_r[mine, :] = up_s[fs]

    def ag_copy(s, d, core, k, dev):
        i = of(s)
        p = at_x(d)
        return rc(X.at[i, p, core], X.at[i, p, core], ag.at[s * 7 + k], xr.at[i * 8 + p * 2 + core], dev)

    def ag_wait(s, d, core):
        ag_copy(s, d, core, 0, sib).wait_recv()

    def ahead(s):
        return 1 + 2 * (s % 2)

    @pl.loop(0, 20)
    def _(t):
        @pl.when(t < 16)
        def _():
            @pl.when(t > 0)
            def _():
                ag_wait(t, 0, c)

            ag_copy(t, 0, c, 0, (fs, lane(1, c))).start()
            ag_copy(t, 0, c, 1, (fs, lane(3, c))).start()
            ag_copy(t, 0, c, 2, sib).start()

        @pl.when(jnp.logical_and(t >= 4, t < 19 - EARLY))
        def _():
            gate_copy(t - 3 + EARLY).start()

        @pl.when(t >= 5)
        def _():
            up_copy(t - 4).start()

        @pl.when(jnp.logical_and(t >= 2, t < 18))
        def _():
            s = t - 2
            da = ahead(s)
            ag_wait(s, 4 - da, c)
            ag_copy(s, 4 - da, c, 3, (fs, lane(da, c))).start()
            ag_copy(s, 4 - da, c, 4, sib).start()
            ag_wait(s, da, c)
            ag_copy(s, da, c, 5, sib).start()

        @pl.when(t >= 4)
        def _():
            s = t - 4
            ag_wait(s, 2, c)
            ag_copy(s, 2, c, 6, sib).start()

    @pl.loop(0, 16)
    def _(s):
        i = of(s)

        @pl.when(s > 0)
        def _():
            rc(down_s.at[0], DN.at[i], es.at[0], er.at[i], sib).wait_recv()

        @pl.when(i // 2 != tp)
        def _():
            down_on(i).start()

        @pl.when(i // 2 == tp)
        def _():
            down_r[i % 2, tp] = DN[i]

    @pl.loop(1, 16)
    def _(s):
        i = of(s)
        rows = pl.ds(pl.multiple_of(i * 128, 128), 128)
        rc(gate_s.at[0], gate_r.at[rows], gs.at[0], gr.at[i], sib).wait_recv()
        rc(up_s.at[0], up_r.at[rows], us.at[0], ur.at[i], sib).wait_recv()

    o_gate = pltpu.make_async_copy(gate_r, gate_o.at[0], osem.at[16])
    o_up = pltpu.make_async_copy(up_r, up_o.at[0], osem.at[17])
    o_gate.start()
    o_up.start()

    @pl.loop(0, 16)
    def _(k):
        @pl.when(k % 8 != tp)
        def _():
            rc(DN.at[0], down_r.at[k // 8, k % 8], ds.at[0], dr.at[k], sib).wait_recv()

    def o_down(k):
        h, j = k // 8, k % 8
        return pltpu.make_async_copy(
            down_r.at[h, j], down_o.at[0, pl.ds(h * 256, 256), pl.ds(j * 256, 256)], osem.at[k]
        )

    for k in range(16):
        o_down(k).start()

    acc[...] = jnp.zeros_like(acc)

    def pair_copy(s):
        return rc(X.at[of(s), :, oc], RB.at[s], dds.at[s], ddr.at[s], sib)

    def far_copy(s):
        return rc(X.at[of(s), at_x(2), c], D2.at[s], s2s.at[s], s2r.at[s], (fs, lane(ahead(s), c)))

    def a_copy(s):
        return rc(
            X.at[of(s), at_x(ahead(s)), c], FA.at[s], sas.at[s], sar.at[s], (fs, lane(ahead(s), c))
        )

    def b_copy(s):
        return rc(
            X.at[of(s), at_x(4 - ahead(s)), c], FB.at[s], sbs.at[s], sbr.at[s], (fs, lane(4 - ahead(s), c))
        )

    def ret_copy(s):
        return rc(X.at[of(s), x, c], RET.at[fs], rts.at[s], rtr.at[fs], (of(s), tp))

    LAGS = (0, 2, 5, 8, 11)

    def stage(t, k, low=0):
        s = t - LAGS[k]
        return jnp.logical_and(s >= low, s < 16), s

    @pl.loop(0, 16 + LAGS[4])
    def _(t):
        on4, s4 = stage(t, 4)
        on3, s3 = stage(t, 3)
        on2, s2 = stage(t, 2)
        on1, s1 = stage(t, 1)
        on0, s0 = stage(t, 0)

        @pl.when(on2)
        def _():
            far_copy(s2).wait_recv()
            i, p = of(s2), at_x(ahead(s2))
            X[i, p, c] = (X[i, p, c].astype(F32) + D2[s2].astype(F32)).astype(BF)

        @pl.when(on1)
        def _():
            pair_copy(s1).wait_recv()
            i = of(s1)
            for d in (2, 4 - ahead(s1), ahead(s1), 0):
                p = at_x(d)
                X[i, p, c] = (X[i, p, c].astype(F32) + RB[s1, p].astype(F32)).astype(BF)

        @pl.when(on2)
        def _():
            a_copy(s2).start()

        @pl.when(on1)
        def _():
            far_copy(s1).start()
            b_copy(s1).start()

        @pl.when(on3)
        def _():
            a_copy(s3).wait_recv()
            b_copy(s3).wait_recv()
            i = of(s3)
            X[i, x, c] = (X[i, x, c].astype(F32) + FA[s3].astype(F32) + FB[s3].astype(F32)).astype(BF)

        @pl.when(on0)
        def _():
            for k in range(7):
                ag_copy(s0, 0, c, k, sib).wait_send()
            i = of(s0)
            for d in range(4):
                ag_wait(s0, d, oc)
            rows = jnp.concatenate([X[i, p // 2, p % 2] for p in range(8)], axis=1)
            for h in range(2):
                g = jnp.dot(rows, gate_r[:, h * 256 : h * 256 + 256], preferred_element_type=F32)
                u = jnp.dot(rows, up_r[:, h * 256 : h * 256 + 256], preferred_element_type=F32)
                H[h] = (g / (1.0 + jnp.exp(-g)) * u).astype(BF)
            hid = jnp.concatenate([H[0], H[1]], axis=1)
            for j in range(8):
                w = jnp.concatenate([down_r[0, j], down_r[1, j]], axis=0)
                X[i, j // 2, j % 2] = jnp.dot(hid, w, preferred_element_type=F32).astype(BF)

        @pl.when(on3)
        def _():
            @pl.when(s3 > 0)
            def _():
                ret_copy(s3).start()

            @pl.when(s3 == 0)
            def _():
                RET[fs] = X[fs, x, c]

        @pl.when(on0)
        def _():
            pair_copy(s0).start()

        @pl.when(on4)
        def _():
            e = to(s4)

            @pl.when(s4 > 0)
            def _():
                rc(X.at[0, 0, 0], RET.at[e], rts.at[0], rtr.at[e], sib).wait_recv()

            want = lax.broadcasted_iota(jnp.int32, (768, CAP), 1) + e * CAP
            k0 = cols[:, 0:1].astype(jnp.int32)
            k1 = cols[:, 1:2].astype(jnp.int32)
            w = jnp.where(want == k0, cols[:, 2:3], jnp.where(want == k1, cols[:, 3:4], 0.0))
            hi = w.astype(BF)
            lo = (w - hi.astype(F32)).astype(BF)
            back = RET[e]
            acc[...] += jnp.dot(hi, back, preferred_element_type=F32) + jnp.dot(
                lo, back, preferred_element_type=F32
            )

    out_ref[...] = acc[...].astype(BF)

    o_gate.wait()
    o_up.wait()
    for k in range(16):
        o_down(k).wait()

    @pl.loop(1, 16)
    def _(s):
        gate_copy(s).wait_send()
        up_copy(s).wait_send()
        down_copy(s).wait_send()
        disp_copy(s).wait_send()
        ret_copy(s).wait_send()

    @pl.loop(0, 16)
    def _(i):
        @pl.when(i // 2 != tp)
        def _():
            down_on(i).wait_send()

    @pl.loop(0, 16)
    def _(s):
        pair_copy(s).wait_send()
        far_copy(s).wait_send()
        a_copy(s).wait_send()
        b_copy(s).wait_send()


def settle(*refs):
    src, dst, bufs, (rd, wr) = refs[:4], refs[4:8], refs[8:12], refs[12:]
    parts = [(k, h) for h in range(2) for k in range(4)]

    def half(k, h, ref):
        ref = ref.at[0] if k < 3 else ref
        n = (1024, 1024, 256, 384)[k]
        return ref.at[h * n : h * n + n]

    def get(n):
        k, h = parts[n]
        return pltpu.make_async_copy(half(k, h, src[k]), half(k, h, bufs[k]), rd.at[n])

    def put(n):
        k, h = parts[n]
        return pltpu.make_async_copy(half(k, h, bufs[k]), half(k, h, dst[k]), wr.at[n])

    for n in range(8):
        get(n).start()
    for n in range(8):
        get(n).wait()
        put(n).start()
    for n in range(8):
        put(n).wait()


def body(tokens, routes, route_weight, norm_gain, gate_master, up_master, down_master):
    hbm = pl.BlockSpec(memory_space=pl.ANY)
    vm = pl.BlockSpec(memory_space=pltpu.VMEM)
    dma = pltpu.SemaphoreType.DMA
    piece = (16, CAP, 256)
    held = tuple(
        pl.pallas_call(
            kernel,
            name="experts",
            out_shape=(
                jax.ShapeDtypeStruct((1, 2048, 512), BF),
                jax.ShapeDtypeStruct((1, 2048, 512), BF),
                jax.ShapeDtypeStruct((1, 512, 2048), BF),
                jax.ShapeDtypeStruct((768, 256), BF),
            ),
            in_specs=[hbm, vm, vm, vm, hbm, hbm, hbm],
            out_specs=(hbm, hbm, hbm, vm),
            scratch_shapes=[
                pltpu.VMEM((16, 4, 2, CAP, 256), BF),
                pltpu.VMEM((16, 4, CAP, 256), BF),
                pltpu.VMEM(piece, BF),
                pltpu.VMEM(piece, BF),
                pltpu.VMEM(piece, BF),
                pltpu.VMEM(piece, BF),
                pltpu.VMEM(piece, BF),
                pltpu.VMEM((2, CAP, 256), BF),
                pltpu.VMEM((16, 128, 512), BF),
                pltpu.VMEM((16, 128, 512), BF),
                pltpu.VMEM((16, 256, 256), BF),
                pltpu.VMEM((2048, 512), BF),
                pltpu.VMEM((2048, 512), BF),
                pltpu.VMEM((2, 8, 256, 256), BF),
                pltpu.VMEM((16, 256, 256), BF),
                pltpu.VMEM((16, 128, 512), F32),
                pltpu.VMEM((16, 256, 256), F32),
                pltpu.VMEM((768, 2048), BF),
                pltpu.VMEM((768, 256), BF),
                pltpu.VMEM((768, 256), F32),
                pltpu.VMEM((16, 768), F32),
                pltpu.VMEM((768, 128), F32),
                dma((4,)),
                *[dma((16,))] * 9,
                dma((128,)),
                dma((112,)),
                *[dma((16,))] * 10,
                dma((18,)),
            ],
            compiler_params=pltpu.CompilerParams(
                collective_id=0, has_side_effects=True, vmem_limit_bytes=67043328
            ),
        )(
            tokens,
            routes.T,
            route_weight.T,
            norm_gain.reshape(1, 128),
            gate_master,
            up_master,
            down_master,
        )
    )
    shapes = tuple(jax.ShapeDtypeStruct(v.shape, v.dtype) for v in held)
    return tuple(
        pl.pallas_call(
            settle,
            name="settle",
            out_shape=shapes,
            in_specs=[hbm] * 4,
            out_specs=(hbm,) * 4,
            scratch_shapes=[*[pltpu.VMEM(v.shape, v.dtype) for v in held], dma((8,)), dma((8,))],
        )(*held)
    )


def solution(mesh):
    placed = (
        P("fs", None),
        P("fs", None),
        P("fs", None),
        P("fs"),
        P(None, "fs", "tp"),
        P(None, "fs", "tp"),
        P(None, "fs", "tp"),
    )
    return jax.shard_map(
        body,
        mesh=mesh,
        in_specs=placed,
        out_specs=(P("fs", None, "tp"), P("fs", None, "tp"), P("fs", "tp", None), P("fs", "tp")),
        check_vma=False,
    )
```

```python
import functools

import jax
import jax.numpy as jnp
from jax import lax
from jax.experimental import pallas as pl
from jax.experimental.pallas import tpu as pltpu
from jax.sharding import PartitionSpec as P

CAP = 216
MESH = pl.DeviceIdType.MESH
BF = jnp.bfloat16
F32 = jnp.float32
EARLY = 7


def kernel(
    tok_h, rt_ref, wt_ref, gain_ref, gate_h, up_h, down_h,
    gate_r, up_r, down_r, out_ref,
    X, RB, D2, FA, FB, RET, PS, H,
    gate_s, up_s, down_s,
    DN, st_a, st_d, tok, nrm, acc, pos_e, cols,
    ld, gs, gr, us, ur, ds, dr, es, er, ps, xr, ag,
    dds, ddr, s2s, s2r, sas, sar, sbs, sbr, rts, rtr,
):
    fs, tp = lax.axis_index("fs"), lax.axis_index("tp")
    z, y = fs // 4, fs % 4
    x, c = tp // 2, tp % 2
    oc = 1 - c

    def to(s):
        dy = s % 4
        dz = (s // 4 + dy) % 4
        return ((z + dz) % 4) * 4 + (y + dy) % 4

    def of(s):
        dy = s % 4
        dz = (s // 4 + dy) % 4
        return ((z + 4 - dz) % 4) * 4 + (y + 4 - dy) % 4

    def at_x(d):
        return (x + d) % 4

    def lane(d, core):
        return at_x(d) * 2 + core

    sib = (fs, x * 2 + oc)

    def rc(src, dst, ss, rs, dev):
        return pltpu.make_async_remote_copy(
            src_ref=src, dst_ref=dst, send_sem=ss, recv_sem=rs, device_id=dev, device_id_type=MESH
        )

    l_gate = pltpu.make_async_copy(gate_h, st_a, ld.at[0])
    l_tok = pltpu.make_async_copy(tok_h, tok, ld.at[1])
    l_down = pltpu.make_async_copy(down_h, st_d, ld.at[2])
    l_up = pltpu.make_async_copy(up_h, st_a, ld.at[3])
    l_gate.start()
    l_tok.start()
    l_down.start()

    bar = pltpu.get_barrier_semaphore()

    def sig(dev):
        pl.semaphore_signal(bar, inc=1, device_id=dev, device_id_type=MESH)

    @pl.loop(1, 16)
    def _(s):
        sig((to(s), tp))

    @pl.loop(1, 8)
    def _(k):
        sig((fs, (tp + k) % 8))

    e_id = lax.broadcasted_iota(jnp.int32, (16, 768), 0)
    m0 = e_id == rt_ref[0:1, :]
    m1 = e_id == rt_ref[1:2, :]
    mt = jnp.logical_or(m0, m1)
    before = (
        lax.broadcasted_iota(jnp.int32, (768, 768), 0) < lax.broadcasted_iota(jnp.int32, (768, 768), 1)
    )
    count = jnp.dot(
        jnp.where(mt, 1.0, 0.0).astype(BF), jnp.where(before, 1.0, 0.0).astype(BF), preferred_element_type=F32
    )
    pos_e[...] = jnp.where(mt, count, -1.0)
    slot = count + (e_id * CAP).astype(F32)
    slot0 = jnp.sum(jnp.where(m0, slot, 0.0), axis=0, keepdims=True)
    slot1 = jnp.sum(jnp.where(m1, slot, 0.0), axis=0, keepdims=True)
    row = lax.broadcasted_iota(jnp.int32, (128, 768), 0)
    table = jnp.where(
        row == 0, slot0, jnp.where(row == 1, slot1, jnp.where(row == 2, wt_ref[0:1, :], wt_ref[1:2, :]))
    )
    cols[...] = table.T

    r128 = lax.broadcasted_iota(jnp.int32, (128, 128), 0)
    c128 = lax.broadcasted_iota(jnp.int32, (128, 128), 1)
    gain = jnp.sum(jnp.where(r128 == c128, gain_ref[...], 0.0), axis=1, keepdims=True)
    mine = pl.ds(pl.multiple_of(fs * 128, 128), 128)

    l_gate.wait()

    @pl.loop(0, 16)
    def _(e):
        gate_s[e] = (st_a[e] * gain).astype(BF)

    gate_r[mine, :] = gate_s[fs]
    l_up.start()

    pl.semaphore_wait(bar, 22)

    def gate_copy(s):
        return rc(gate_s.at[to(s)], gate_r.at[mine], gs.at[s], gr.at[fs], (to(s), tp))

    def up_copy(s):
        return rc(up_s.at[to(s)], up_r.at[mine], us.at[s], ur.at[fs], (to(s), tp))

    def down_copy(s):
        return rc(down_s.at[to(s)], DN.at[fs], es.at[s], er.at[fs], (to(s), tp))

    def down_at(h, j):
        return down_r.at[
            pl.ds(pl.multiple_of(h * 256, 256), 256), pl.ds(pl.multiple_of(j * 256, 256), 256)
        ]

    def down_on(i):
        return rc(DN.at[i], down_at(i % 2, tp), ds.at[i], dr.at[(i % 2) * 8 + tp], (fs, i // 2))

    @pl.loop(1, 1 + EARLY)
    def _(s):
        gate_copy(s).start()

    l_tok.wait()
    share = pl.ds(pl.multiple_of(tp * 256, 256), 256)

    @pl.loop(0, 12)
    def _(r):
        rows = pl.ds(pl.multiple_of(r * 64, 64), 64)
        v = tok[rows, :].astype(F32)
        inv = lax.rsqrt(jnp.mean(v * v, axis=-1, keepdims=True) + 1e-06)
        nrm[rows, :] = (tok[rows, share].astype(F32) * inv).astype(BF)

    s_id = lax.broadcasted_iota(jnp.int32, (CAP, 768), 0).astype(F32)

    def block(e):
        pick = jnp.where(s_id == pos_e[pl.ds(e, 1), :], 1.0, 0.0).astype(BF)
        return jnp.dot(pick, nrm[...], preferred_element_type=F32).astype(BF)

    def disp_copy(s):
        return rc(PS.at[s], X.at[fs, x, c], ps.at[s], xr.at[fs * 8 + tp], (to(s), tp))

    X[fs, x, c] = block(fs)

    @pl.loop(1, 17)
    def _(s):
        @pl.when(s < 16)
        def _():
            PS[s] = block(to(s))

        @pl.when(s > 1)
        def _():
            disp_copy(s - 1).start()

    l_down.wait()

    @pl.loop(0, 16)
    def _(e):
        down_s[e] = st_d[e].astype(BF)

    @pl.loop(1, 16)
    def _(s):
        down_copy(s).start()

    DN[fs] = down_s[fs]

    l_up.wait()

    @pl.loop(0, 16)
    def _(e):
        up_s[e] = (st_a[e] * gain).astype(BF)

    up_r[mine, :] = up_s[fs]

    def ag_copy(s, d, core, k, dev):
        i = of(s)
        p = at_x(d)
        return rc(X.at[i, p, core], X.at[i, p, core], ag.at[s * 7 + k], xr.at[i * 8 + p * 2 + core], dev)

    def ag_wait(s, d, core):
        ag_copy(s, d, core, 0, sib).wait_recv()

    def ahead(s):
        return 1 + 2 * ((s + c) % 2)

    @pl.loop(0, 20)
    def _(t):
        @pl.when(t < 16)
        def _():
            @pl.when(t > 0)
            def _():
                ag_wait(t, 0, c)

            ag_copy(t, 0, c, 0, (fs, lane(1, c))).start()
            ag_copy(t, 0, c, 1, (fs, lane(3, c))).start()
            ag_copy(t, 0, c, 2, sib).start()

        @pl.when(jnp.logical_and(t >= 4, t < 19 - EARLY))
        def _():
            gate_copy(t - 3 + EARLY).start()

        @pl.when(t >= 5)
        def _():
            up_copy(t - 4).start()

        @pl.when(jnp.logical_and(t >= 2, t < 18))
        def _():
            s = t - 2
            da = ahead(s)
            ag_wait(s, 4 - da, c)
            ag_copy(s, 4 - da, c, 3, (fs, lane(da, c))).start()
            ag_copy(s, 4 - da, c, 4, sib).start()
            ag_wait(s, da, c)
            ag_copy(s, da, c, 5, sib).start()

        @pl.when(t >= 4)
        def _():
            s = t - 4
            ag_wait(s, 2, c)
            ag_copy(s, 2, c, 6, sib).start()

    @pl.loop(0, 16)
    def _(s):
        i = of(s)

        @pl.when(s > 0)
        def _():
            rc(down_s.at[0], DN.at[i], es.at[0], er.at[i], sib).wait_recv()

        @pl.when(i // 2 != tp)
        def _():
            down_on(i).start()

        @pl.when(i // 2 == tp)
        def _():
            down_at(i % 2, tp)[...] = DN[i]

    @pl.loop(1, 16)
    def _(s):
        i = of(s)
        rows = pl.ds(pl.multiple_of(i * 128, 128), 128)
        rc(gate_s.at[0], gate_r.at[rows], gs.at[0], gr.at[i], sib).wait_recv()
        rc(up_s.at[0], up_r.at[rows], us.at[0], ur.at[i], sib).wait_recv()

    @pl.loop(0, 16)
    def _(k):
        @pl.when(k % 8 != tp)
        def _():
            rc(DN.at[0], down_at(k // 8, k % 8), ds.at[0], dr.at[k], sib).wait_recv()

    acc[...] = jnp.zeros_like(acc)

    def pair_copy(s):
        return rc(X.at[of(s), :, oc], RB.at[s], dds.at[s], ddr.at[s], sib)

    def far_copy(s):
        return rc(X.at[of(s), at_x(2), c], D2.at[s], s2s.at[s], s2r.at[s], (fs, lane(ahead(s), c)))

    def a_copy(s):
        return rc(
            X.at[of(s), at_x(ahead(s)), c], FA.at[s], sas.at[s], sar.at[s], (fs, lane(ahead(s), c))
        )

    def b_copy(s):
        return rc(
            X.at[of(s), at_x(4 - ahead(s)), c], FB.at[s], sbs.at[s], sbr.at[s], (fs, lane(4 - ahead(s), c))
        )

    def ret_copy(s):
        return rc(X.at[of(s), x, c], RET.at[fs], rts.at[s], rtr.at[fs], (of(s), tp))

    LAGS = (0, 2, 5, 8, 11)

    def stage(t, k, low=0):
        s = t - LAGS[k]
        return jnp.logical_and(s >= low, s < 16), s

    @pl.loop(0, 16 + LAGS[4])
    def _(t):
        on4, s4 = stage(t, 4)
        on3, s3 = stage(t, 3)
        on2, s2 = stage(t, 2)
        on1, s1 = stage(t, 1)
        on0, s0 = stage(t, 0)

        @pl.when(on2)
        def _():
            far_copy(s2).wait_recv()
            i, p = of(s2), at_x(ahead(s2))
            X[i, p, c] = (X[i, p, c].astype(F32) + D2[s2].astype(F32)).astype(BF)

        @pl.when(on1)
        def _():
            pair_copy(s1).wait_recv()
            i = of(s1)
            for d in (2, 4 - ahead(s1), ahead(s1), 0):
                p = at_x(d)
                X[i, p, c] = (X[i, p, c].astype(F32) + RB[s1, p].astype(F32)).astype(BF)

        @pl.when(on2)
        def _():
            a_copy(s2).start()

        @pl.when(on1)
        def _():
            far_copy(s1).start()
            b_copy(s1).start()

        @pl.when(on3)
        def _():
            a_copy(s3).wait_recv()
            b_copy(s3).wait_recv()
            i = of(s3)
            X[i, x, c] = (X[i, x, c].astype(F32) + FA[s3].astype(F32) + FB[s3].astype(F32)).astype(BF)

        @pl.when(on0)
        def _():
            for k in range(7):
                ag_copy(s0, 0, c, k, sib).wait_send()
            i = of(s0)
            for d in range(4):
                ag_wait(s0, d, oc)
            rows = jnp.concatenate([X[i, p // 2, p % 2] for p in range(8)], axis=1)
            for h in range(2):
                g = jnp.dot(rows, gate_r[:, h * 256 : h * 256 + 256], preferred_element_type=F32)
                u = jnp.dot(rows, up_r[:, h * 256 : h * 256 + 256], preferred_element_type=F32)
                H[h] = (g / (1.0 + jnp.exp(-g)) * u).astype(BF)
            hid = jnp.concatenate([H[0], H[1]], axis=1)
            for j in range(8):
                w = down_r[:, j * 256 : j * 256 + 256]
                X[i, j // 2, j % 2] = jnp.dot(hid, w, preferred_element_type=F32).astype(BF)

        @pl.when(on3)
        def _():
            @pl.when(s3 > 0)
            def _():
                ret_copy(s3).start()

            @pl.when(s3 == 0)
            def _():
                RET[fs] = X[fs, x, c]

        @pl.when(on0)
        def _():
            pair_copy(s0).start()

        @pl.when(on4)
        def _():
            e = to(s4)

            @pl.when(s4 > 0)
            def _():
                rc(X.at[0, 0, 0], RET.at[e], rts.at[0], rtr.at[e], sib).wait_recv()

            want = lax.broadcasted_iota(jnp.int32, (768, CAP), 1) + e * CAP
            k0 = cols[:, 0:1].astype(jnp.int32)
            k1 = cols[:, 1:2].astype(jnp.int32)
            w = jnp.where(want == k0, cols[:, 2:3], jnp.where(want == k1, cols[:, 3:4], 0.0))
            hi = w.astype(BF)
            lo = (w - hi.astype(F32)).astype(BF)
            back = RET[e]
            acc[...] += jnp.dot(hi, back, preferred_element_type=F32) + jnp.dot(
                lo, back, preferred_element_type=F32
            )

    out_ref[...] = acc[...].astype(BF)

    @pl.loop(1, 16)
    def _(s):
        gate_copy(s).wait_send()
        up_copy(s).wait_send()
        down_copy(s).wait_send()
        disp_copy(s).wait_send()
        ret_copy(s).wait_send()

    @pl.loop(0, 16)
    def _(i):
        @pl.when(i // 2 != tp)
        def _():
            down_on(i).wait_send()

    @pl.loop(0, 16)
    def _(s):
        pair_copy(s).wait_send()
        far_copy(s).wait_send()
        a_copy(s).wait_send()
        b_copy(s).wait_send()


def settle(gate_v, up_v, down_v, out_v, gate_o, up_o, down_o, out_o, sem):
    copies = [
        pltpu.make_async_copy(gate_v, gate_o.at[0], sem.at[0]),
        pltpu.make_async_copy(up_v, up_o.at[0], sem.at[1]),
        pltpu.make_async_copy(down_v, down_o.at[0], sem.at[2]),
        pltpu.make_async_copy(out_v, out_o, sem.at[3]),
    ]
    for copy in copies:
        copy.start()
    for copy in copies:
        copy.wait()


def body(tokens, routes, route_weight, norm_gain, gate_master, up_master, down_master):
    hbm = pl.BlockSpec(memory_space=pl.ANY)
    vm = pl.BlockSpec(memory_space=pltpu.VMEM)
    dma = pltpu.SemaphoreType.DMA
    piece = (16, CAP, 256)
    gate_serve, up_serve, down_serve, layer_out = (
        pl.pallas_call(
            kernel,
            name="experts",
            out_shape=(
                pltpu.VMEM((2048, 512), BF),
                pltpu.VMEM((2048, 512), BF),
                pltpu.VMEM((512, 2048), BF),
                pltpu.VMEM((768, 256), BF),
            ),
            in_specs=[hbm, vm, vm, vm, hbm, hbm, hbm],
            out_specs=(vm, vm, vm, vm),
            scratch_shapes=[
                pltpu.VMEM((16, 4, 2, CAP, 256), BF),
                pltpu.VMEM((16, 4, CAP, 256), BF),
                pltpu.VMEM(piece, BF),
                pltpu.VMEM(piece, BF),
                pltpu.VMEM(piece, BF),
                pltpu.VMEM(piece, BF),
                pltpu.VMEM(piece, BF),
                pltpu.VMEM((2, CAP, 256), BF),
                pltpu.VMEM((16, 128, 512), BF),
                pltpu.VMEM((16, 128, 512), BF),
                pltpu.VMEM((16, 256, 256), BF),
                pltpu.VMEM((16, 256, 256), BF),
                pltpu.VMEM((16, 128, 512), F32),
                pltpu.VMEM((16, 256, 256), F32),
                pltpu.VMEM((768, 2048), BF),
                pltpu.VMEM((768, 256), BF),
                pltpu.VMEM((768, 256), F32),
                pltpu.VMEM((16, 768), F32),
                pltpu.VMEM((768, 128), F32),
                dma((4,)),
                *[dma((16,))] * 9,
                dma((128,)),
                dma((112,)),
                *[dma((16,))] * 10,
            ],
            compiler_params=pltpu.CompilerParams(
                collective_id=0, has_side_effects=True, vmem_limit_bytes=60000000
            ),
        )(
            tokens,
            routes.T,
            route_weight.T,
            norm_gain.reshape(1, 128),
            gate_master,
            up_master,
            down_master,
        )
    )
    held = [
        pltpu.with_memory_space_constraint(v, pltpu.VMEM)
        for v in (gate_serve, up_serve, down_serve, layer_out)
    ]
    return tuple(
        pl.pallas_call(
            settle,
            name="settle",
            out_shape=(
                jax.ShapeDtypeStruct((1, 2048, 512), BF),
                jax.ShapeDtypeStruct((1, 2048, 512), BF),
                jax.ShapeDtypeStruct((1, 512, 2048), BF),
                jax.ShapeDtypeStruct((768, 256), BF),
            ),
            in_specs=[vm] * 4,
            out_specs=(hbm,) * 4,
            scratch_shapes=[dma((4,))],
            compiler_params=pltpu.CompilerParams(vmem_limit_bytes=1 << 20),
        )(*held)
    )


def solution(mesh):
    placed = (
        P("fs", None),
        P("fs", None),
        P("fs", None),
        P("fs"),
        P(None, "fs", "tp"),
        P(None, "fs", "tp"),
        P(None, "fs", "tp"),
    )
    return jax.shard_map(
        body,
        mesh=mesh,
        in_specs=placed,
        out_specs=(P("fs", None, "tp"), P("fs", None, "tp"), P("fs", "tp", None), P("fs", "tp")),
        check_vma=False,
    )
```
